32 devices in a mesh: sp: 16 (over z, y, x), tp: 2 (over core).
Axes of the slice: x: 2, y: 2, z: 4, core: 2. Of those that a mesh axis runs over, the one named last changes fastest.
Arguments:
- latent: bfloat16 [4096, 2048], P(('sp', 'tp')), may hold values from -6 to 6
- context: bfloat16 [512, 2048], P('sp'), may hold values from -6 to 6
- condition: float32 [2048], P('tp'), may hold values from -6 to 6
- context_condition: float32 [2048], P('tp'), may hold values from -6 to 6
- modulation_weight: bfloat16 [2048, 6144], P('tp', 'sp'), may hold values from -0.125 to 0.125
- query_first: bfloat16 [2048, 512], P(None, 'tp'), may hold values from -1 to 1
- query_second: bfloat16 [2048, 512], P(None, 'tp'), may hold values from -1 to 1
- key_first: bfloat16 [2048, 512], P(None, 'tp'), may hold values from -1 to 1
- key_second: bfloat16 [2048, 512], P(None, 'tp'), may hold values from -1 to 1
- value_weight: bfloat16 [2048, 1024], P(None, 'tp'), may hold values from -0.125 to 0.125
- lambda_head: float32 [8], P('tp'), may hold values from 0.3 to 0.8
- context_score_boost: float32 [8], P('tp'), may hold values from 1.5 to 3
- head_gain: float32 [128], replicated, may hold values from 0.1 to 1.9
- output_weight: bfloat16 [1024, 2048], P('tp'), may hold values from -0.1875 to 0.1875
Outputs:
- updated: bfloat16 [4096, 2048], P(('sp', 'tp'))
The draws below stay inside these ranges and needn't reach their ends.
All inputs are finite; a program needn't handle non-finite values.
Results may differ from the reference program's by a relative error of at most 0.0095.
Values may be sent and summed in bfloat16 or wider, within the bound.
A program may use at most 64 MiB of HBM per device.

```python
import jax
import jax.numpy as jnp
from jax import lax

D = 2048
HEADS = 8
HEAD_DIM = 64
VALUE_DIM = 128
GRID_W = 64
CTX = 512
TOKENS = 4096


def drawn_weight(key, stream):
    jitter = jax.random.normal(jax.random.fold_in(key, stream), (D, HEADS * HEAD_DIM), jnp.float32)
    return jnp.clip(jitter, -6.0, 6.0) * D ** (-0.5)


def draw_latent(key, part):
    jitter = jax.random.normal(jax.random.fold_in(key, 21), (TOKENS, D), jnp.float32)
    result = jnp.clip(jitter, -6.0, 6.0)
    return result.astype(jnp.bfloat16)


def draw_query_first(key, part):
    result = drawn_weight(key, 31)
    return jnp.clip(result, -1.0, 1.0).astype(jnp.bfloat16)


def draw_key_first(key, part):
    result = drawn_weight(key, 32)
    return jnp.clip(result, -1.0, 1.0).astype(jnp.bfloat16)


def draw_query_second(key, part):
    result = drawn_weight(key, 33)
    return jnp.clip(result, -1.0, 1.0).astype(jnp.bfloat16)


def draw_key_second(key, part):
    result = drawn_weight(key, 34)
    return jnp.clip(result, -1.0, 1.0).astype(jnp.bfloat16)


def shard_levels(stream_key, extent, cuts, smallest, largest):
    def one(position, shards_of):
        draws = jax.random.uniform(jax.random.fold_in(jax.random.fold_in(stream_key, 6), position), (shards_of,), jnp.float32, smallest / len(cuts), largest / len(cuts))
        return jnp.repeat(jnp.exp(draws), extent[position] // shards_of).reshape((-1,) + (1,) * (len(extent) - position - 1))

    factor_of = one(*cuts[0])
    for cut in cuts[1:]:
        factor_of = factor_of * one(*cut)
    return factor_of


def gaussian(stream_key, dims, scale, limit, split=(), kind=jnp.bfloat16):
    loudness = shard_levels(stream_key, dims, split, -0.22, 0.18) if split else 1.0
    values = jax.random.normal(stream_key, dims, jnp.float32) * scale * loudness
    return jnp.minimum(jnp.maximum(values, -limit), limit).astype(kind)


def setup_inputs(seed: int = 0) -> dict:
    key_list = jax.random.split(jax.random.key(seed), 15)
    latent = draw_latent(jax.random.fold_in(key_list[14], 71), 0)
    context = gaussian(key_list[1], (CTX, D), 1.0, 6.0, ((0, 16),))
    condition = gaussian(key_list[2], (D,), 1.0, 6.0, ((0, 2),), jnp.float32)
    context_condition = gaussian(key_list[3], (D,), 1.0, 6.0, ((0, 2),), jnp.float32)
    modulation_weight = gaussian(key_list[4], (D, 3 * D), D ** -0.5, 0.125, ((0, 2), (1, 16)))
    query_first = draw_query_first(jax.random.fold_in(key_list[14], 71), 0)
    query_second = draw_query_second(jax.random.fold_in(key_list[14], 71), 0)
    key_first = draw_key_first(jax.random.fold_in(key_list[14], 71), 0)
    key_second = draw_key_second(jax.random.fold_in(key_list[14], 71), 0)
    value_weight = gaussian(key_list[9], (D, HEADS * VALUE_DIM), D ** -0.5, 0.125, ((1, 2),))
    lambda_head = jnp.clip(0.3 + 0.5 * jax.random.uniform(key_list[10], (HEADS,), jnp.float32) ** shard_levels(key_list[10], (HEADS,), ((0, 2),), -0.2, 0.2), 0.3, 0.8)
    context_score_boost = jnp.clip(1.5 + 1.5 * jax.random.uniform(key_list[11], (HEADS,), jnp.float32) ** shard_levels(key_list[11], (HEADS,), ((0, 2),), -0.2, 0.2), 1.5, 3.0)
    head_gain = jnp.clip(1.0 + 0.18 * jax.random.normal(key_list[12], (VALUE_DIM,), jnp.float32), 0.1, 1.9)
    output_weight = gaussian(key_list[13], (HEADS * VALUE_DIM, D), (HEADS * VALUE_DIM) ** -0.5, 0.1875, ((0, 2),))
    return {"latent": latent, "context": context, "condition": condition, "context_condition": context_condition, "modulation_weight": modulation_weight, "query_first": query_first, "query_second": query_second, "key_first": key_first, "key_second": key_second, "value_weight": value_weight, "lambda_head": lambda_head, "context_score_boost": context_score_boost, "head_gain": head_gain, "output_weight": output_weight}


EPSILON = 1e-06
THETA = 10000.0

def norm_rows(rows):
    values = rows.astype(jnp.float32)
    return values * lax.rsqrt(lax.optimization_barrier(jnp.mean(values * values, axis=-1, keepdims=True)) + EPSILON)

def rotate_pairs(values, positions):
    half = values.shape[-1] // 2
    quarter = half // 2
    reciprocal_norm = THETA ** (-jnp.arange(quarter, dtype=jnp.float32) / quarter)

    def turn(part, where):
        angle = where.astype(jnp.float32)[:, None] * reciprocal_norm[None, :]
        cosine_table = jnp.concatenate([jnp.cos(angle)] * 2, -1)[:, None, :]
        sine = jnp.concatenate([jnp.sin(angle)] * 2, -1)[:, None, :]
        flipped = jnp.concatenate([-part[..., quarter:], part[..., :quarter]], -1)
        return part * cosine_table + flipped * sine
    grid_row = positions // GRID_W
    grid_col = positions % GRID_W
    return jnp.concatenate([turn(values[..., :half], grid_row), turn(values[..., half:], grid_col)], -1)

def project(rows, weight):
    return jnp.dot(rows, weight, preferred_element_type=jnp.float32).reshape(rows.shape[0], HEADS, -1)

def reference(latent, context, condition, context_condition, modulation_weight, query_first, query_second, key_first, key_second, value_weight, lambda_head, context_score_boost, head_gain, output_weight):
    signal = jax.nn.silu(jnp.stack([condition, context_condition])).astype(jnp.bfloat16)
    modulation = jnp.dot(signal, modulation_weight, preferred_element_type=jnp.float32)
    shift = modulation[:, :D]
    scale = modulation[:, D:2 * D]
    gate = modulation[:, 2 * D:]
    h_latent = (norm_rows(latent) * (1.0 + scale[0]) + shift[0]).astype(jnp.bfloat16)
    h_context = (norm_rows(context) * (1.0 + scale[1]) + shift[1]).astype(jnp.bfloat16)
    positions = jnp.arange(TOKENS, dtype=jnp.int32)
    queries_one = rotate_pairs(project(h_latent, query_first), positions).astype(jnp.bfloat16)
    queries_two = rotate_pairs(project(h_latent, query_second), positions).astype(jnp.bfloat16)
    latent_one = rotate_pairs(project(h_latent, key_first), positions).astype(jnp.bfloat16)
    latent_two = rotate_pairs(project(h_latent, key_second), positions).astype(jnp.bfloat16)
    latent_values = project(h_latent, value_weight).astype(jnp.bfloat16)
    context_one = project(h_context, key_first).astype(jnp.bfloat16)
    context_two = project(h_context, key_second).astype(jnp.bfloat16)
    context_values = project(h_context, value_weight).astype(jnp.bfloat16)
    keys_one = jnp.concatenate([context_one, latent_one], 0).astype(jnp.float32)
    keys_two = jnp.concatenate([context_two, latent_two], 0).astype(jnp.float32)
    values_all = jnp.concatenate([context_values, latent_values], 0).astype(jnp.float32)
    lift = jnp.concatenate([jnp.broadcast_to(context_score_boost[:, None], (HEADS, CTX)), jnp.zeros((HEADS, TOKENS), jnp.float32)], 1)[:, None, :]
    block = 256 if TOKENS % 256 == 0 else TOKENS
    count = TOKENS // block

    def attend(pair):
        query_one, query_two = pair
        outcomes = []
        for query, keys in ((query_one, keys_one), (query_two, keys_two)):
            scores = jnp.einsum('qhd,khd->hqk', query.astype(jnp.float32), keys) * HEAD_DIM ** (-0.5) + lift
            highest = lax.optimization_barrier(jnp.max(scores, axis=-1, keepdims=True))
            exp_weights = jnp.exp(scores - highest)
            totals = lax.optimization_barrier(jnp.sum(exp_weights, axis=-1))
            rounded = lax.optimization_barrier(exp_weights.astype(jnp.bfloat16))
            weighted = jnp.einsum('hqk,khe->qhe', rounded.astype(jnp.float32), values_all)
            outcomes.append(weighted / jnp.transpose(totals)[:, :, None])
        return outcomes[0] - lambda_head[None, :, None] * outcomes[1]
    blocks = (queries_one.reshape(count, block, HEADS, HEAD_DIM), queries_two.reshape(count, block, HEADS, HEAD_DIM))
    mixed = lax.map(attend, blocks).reshape(TOKENS, HEADS, VALUE_DIM)
    normed = mixed * lax.rsqrt(lax.optimization_barrier(jnp.mean(mixed * mixed, axis=-1, keepdims=True)) + EPSILON) * head_gain
    heads_out = normed.astype(jnp.bfloat16).reshape(TOKENS, HEADS * VALUE_DIM)
    branch = jnp.dot(heads_out, output_weight, preferred_element_type=jnp.float32)
    return (latent.astype(jnp.float32) + gate[0] * branch).astype(jnp.bfloat16)
```

```python
import functools
import math

import jax
import jax.numpy as jnp
from jax import lax
from jax.experimental import pallas as pl
from jax.experimental.pallas import tpu as pltpu
from jax.sharding import PartitionSpec as P

HEAD_DIM = 64
VALUE_DIM = 128
GRID_W = 64
EPSILON = 1e-06
THETA = 10000.0
NEGATIVE = -1e30
LOG2E = math.log2(math.e)
MESH = pl.DeviceIdType.MESH
BF16 = jnp.bfloat16
F32 = jnp.float32
LANES = 128


def rotation_tables(positions, extra):
    half = HEAD_DIM // 2
    quarter = half // 2
    rates = THETA ** (-jnp.arange(quarter, dtype=F32) / quarter)
    lane = jnp.arange(LANES) % HEAD_DIM
    rate = rates[lane % quarter]
    where = jnp.where(
        (lane < half)[None, :], (positions // GRID_W)[:, None], (positions % GRID_W)[:, None]
    ).astype(F32)
    angle = where * rate[None, :]
    sign = jnp.where(lane % half < quarter, -1.0, 1.0).astype(F32)
    cosine = jnp.concatenate([jnp.cos(angle), jnp.ones((extra, LANES), F32)], 0)
    sine = jnp.concatenate([jnp.sin(angle) * sign[None, :], jnp.zeros((extra, LANES), F32)], 0)
    return cosine, sine


def rotate(x, cosine, sine):
    quarter = HEAD_DIM // 4
    lane = lax.broadcasted_iota(jnp.int32, x.shape, 1)
    ahead = pltpu.roll(x, LANES - quarter, 1)
    behind = pltpu.roll(x, quarter, 1)
    flipped = jnp.where(lane % (2 * quarter) < quarter, ahead, behind)
    return x * cosine + flipped * sine


def normed_rows(rows, scale, shift):
    v = rows.astype(F32)
    v = v * lax.rsqrt(jnp.mean(v * v, axis=-1, keepdims=True) + EPSILON)
    return (v * (1.0 + scale) + shift).astype(BF16)


def kernel(
    dims,
    latent_ref, context_ref, cond_ref, ccond_ref, modw_ref,
    wq1_hbm, wq2_hbm, wk1_hbm, wk2_hbm, wv_hbm,
    lam_ref, boost_ref, gain_ref, wo_hbm, cos_ref, sin_ref,
    out_ref,
    wq1, wq2, wk1, wk2, wv, wo,
    sig, modp, modall, modrow, lat, h,
    qs, kvs, q, kv, mx, den, acc, ho, hr, rsend, rs,
    wsem, mp_s, mp_r, lt_s, lt_r, ma_s, ma_r,
    q_s, q_r, kz_s, kv_s, kv_r, ho_s, ho_r, rs_s, rs_r,
):
    S, T, G, R, B, Cr, cw = dims
    s, t = lax.axis_index("sp"), lax.axis_index("tp")
    g, r = s // R, s % R
    rows, D = latent_ref.shape
    Lr = rows * T
    Cp = context_ref.shape[0]

    def remote(src, dst, send, recv, sp, tp):
        return pltpu.make_async_remote_copy(
            src_ref=src, dst_ref=dst, send_sem=send, recv_sem=recv,
            device_id=(sp, tp), device_id_type=MESH,
        )

    loads = [
        pltpu.make_async_copy(a, b, wsem.at[i])
        for i, (a, b) in enumerate(
            [(wk1_hbm, wk1), (wk2_hbm, wk2), (wv_hbm, wv), (wq1_hbm, wq1), (wq2_hbm, wq2), (wo_hbm, wo)]
        )
    ]
    for load in loads:
        load.start()

    barrier = pltpu.get_barrier_semaphore()

    @pl.loop(1, S)
    def _(i):
        pl.semaphore_signal(barrier, inc=1, device_id=((s + i) % S, t), device_id_type=MESH)

    for i in range(1, T):
        pl.semaphore_signal(barrier, inc=1, device_id=(s, (t + i) % T), device_id_type=MESH)

    for i, ref in enumerate((cond_ref, ccond_ref)):
        v = ref[...]
        sig[i : i + 1, :] = v / (1.0 + jnp.exp(-v))
    modp[t] = jnp.dot(sig[...].astype(BF16), modw_ref[...], preferred_element_type=F32)

    pl.semaphore_wait(barrier, S - 1 + T - 1)

    def part_copy(i):
        return remote(modp.at[t], modp.at[t], mp_s.at[i], mp_r.at[t], s, (t + i) % T)

    def latent_copy(i):
        return remote(latent_ref, lat.at[t], lt_s.at[i], lt_r.at[t], s, (t + i) % T)

    for i in range(1, T):
        part_copy(i).start()
    for i in range(1, T):
        latent_copy(i).start()
    lat[t] = latent_ref[...]
    for i in range(1, T):
        o = (t + i) % T
        remote(modp.at[o], modp.at[o], mp_s.at[i], mp_r.at[o], s, o).wait_recv()
    total = modp[0]
    for i in range(1, T):
        total = total + modp[i]
    modall[s] = total

    def mod_copy(i, src):
        return remote(modall.at[src], modall.at[src], ma_s.at[i], ma_r.at[src], (s + i) % S, t)

    @pl.loop(1, S)
    def _(i):
        mod_copy(i, s).start()

    for i in range(1, T):
        o = (t + i) % T
        remote(lat.at[o], lat.at[o], lt_s.at[i], lt_r.at[o], s, o).wait_recv()

    @pl.loop(1, S)
    def _(i):
        mod_copy(i, (s + i) % S).wait_recv()

    for i in range(S):
        modrow[:, i * cw : (i + 1) * cw] = modall[i][:, :cw]

    step = math.gcd(rows, 32)
    for i in range(T):

        @pl.loop(0, rows // step)
        def _(j):
            at = pl.multiple_of(j * step, step)
            h[pl.ds(i * rows + at, step), :] = normed_rows(
                lat[i, pl.ds(at, step), :], modrow[0:1, D : 2 * D], modrow[0:1, :D]
            )

    h[Lr:, :] = normed_rows(context_ref[...], modrow[1:2, D : 2 * D], modrow[1:2, :D])

    for i in range(3):
        loads[i].wait()
    hh = h[...]
    one = jnp.dot(hh, wk1[...], preferred_element_type=F32)
    two = jnp.dot(hh, wk2[...], preferred_element_type=F32)
    for i in range(G):
        cut = slice(i * HEAD_DIM, (i + 1) * HEAD_DIM)
        pair = jnp.concatenate([one[:, cut], two[:, cut]], axis=1)
        kvs[i, :, :LANES] = rotate(pair, cos_ref[...], sin_ref[...]).astype(BF16)
    val = jnp.dot(hh, wv[...], preferred_element_type=F32)
    for i in range(G):
        kvs[i, :, LANES:] = val[:, i * VALUE_DIM : (i + 1) * VALUE_DIM].astype(BF16)

    def kv_out(i):
        to = (g + i) % G
        return remote(kvs.at[to], kv.at[s], kz_s.at[i], kv_r.at[s], to * R + r, t)

    for i in range(1, G):
        kv_out(i).start()
    kv[s] = kvs[g]

    def forward(i, j):
        src = ((g + G - i) % G) * R + r
        return remote(kv.at[src], kv.at[src], kv_s.at[i, j], kv_r.at[src], g * R + (r + j) % R, t)

    def landed(src):
        remote(kv.at[src], kv.at[src], kz_s.at[0], kv_r.at[src], s, t).wait_recv()

    def forward_all(i):
        @pl.loop(1, R)
        def _(j):
            forward(i, j).start()

    forward_all(0)
    for i in range(3, 5):
        loads[i].wait()
    lh = h[:Lr, :]
    one = jnp.dot(lh, wq1[...], preferred_element_type=F32)
    two = jnp.dot(lh, wq2[...], preferred_element_type=F32)
    for i in range(G):
        cut = slice(i * HEAD_DIM, (i + 1) * HEAD_DIM)
        pair = jnp.concatenate([one[:, cut], two[:, cut]], axis=1)
        turned = rotate(pair, cos_ref[:Lr, :], sin_ref[:Lr, :])
        qs[i] = (turned * (LOG2E * HEAD_DIM**-0.5)).astype(BF16)

    def q_out(i):
        to = (g + i) % G
        return remote(qs.at[to], q.at[g], q_s.at[i], q_r.at[g], to * R + r, t)

    for i in range(1, G):
        q_out(i).start()
    q[g] = qs[g]

    mx[...] = jnp.full(mx.shape, NEGATIVE, F32)
    den[...] = jnp.zeros(den.shape, F32)
    acc[...] = jnp.zeros(acc.shape, F32)
    boost = boost_ref[g] * LOG2E

    for i in range(1, G):
        o = (g + i) % G
        remote(q.at[o], q.at[o], q_s.at[i], q_r.at[o], s, t).wait_recv()

    for i in range(G):
        if i + 1 < G:
            landed(((g + G - i - 1) % G) * R + r)
            forward_all(i + 1)
        base = ((g + G - i) % G) * R

        @pl.loop(1, R)
        def _(j):
            landed(base + (r + j) % R)

        @pl.loop(0, (R // B) * G)
        def _(n):
            at = base + (n // G) * B
            n = n % G
            k_l = kv[pl.ds(at, B), :Lr, :LANES].reshape(B * Lr, LANES)
            v_l = kv[pl.ds(at, B), :Lr, LANES:].reshape(B * Lr, VALUE_DIM)
            k_c = kv[pl.ds(at, B), Lr:, :LANES].reshape(B * Cp, LANES)
            v_c = kv[pl.ds(at, B), Lr:, LANES:].reshape(B * Cp, VALUE_DIM)
            qq = q[n]
            lane = lax.broadcasted_iota(jnp.int32, qq.shape, 1)
            nt = (((1,), (1,)), ((), ()))
            for m in range(2):
                qm = jnp.where(lane // HEAD_DIM == m, qq, jnp.zeros_like(qq))
                s_l = lax.dot_general(qm, k_l, nt, preferred_element_type=F32)
                s_c = lax.dot_general(qm, k_c, nt, preferred_element_type=F32) + boost
                if Cp != Cr:
                    spot = lax.broadcasted_iota(jnp.int32, s_c.shape, 1)
                    s_c = jnp.where(spot % Cp < Cr, s_c, NEGATIVE)
                old = mx[m, n]
                peak = jnp.maximum(
                    old,
                    jnp.maximum(
                        jnp.max(s_l, axis=-1, keepdims=True), jnp.max(s_c, axis=-1, keepdims=True)
                    ),
                )
                p_l = jnp.exp2(s_l - peak)
                p_c = jnp.exp2(s_c - peak)
                alpha = jnp.exp2(old - peak)
                mx[m, n] = peak
                den[m, n] = (
                    alpha * den[m, n]
                    + jnp.sum(p_l, axis=-1, keepdims=True)
                    + jnp.sum(p_c, axis=-1, keepdims=True)
                )
                acc[m, n] = (
                    alpha * acc[m, n]
                    + jnp.dot(p_l.astype(BF16), v_l, preferred_element_type=F32)
                    + jnp.dot(p_c.astype(BF16), v_c, preferred_element_type=F32)
                )

    lam = lam_ref[g]
    gain = gain_ref[...]

    def ho_out(i):
        to = (g + i) % G
        return remote(ho.at[to], hr.at[g], ho_s.at[i], ho_r.at[g], to * R + r, t)

    for i in range(1, G + 1):
        n = (g + i) % G
        mixed = acc[0, n] / den[0, n] - lam * (acc[1, n] / den[1, n])
        mixed = mixed * lax.rsqrt(jnp.mean(mixed * mixed, axis=-1, keepdims=True) + EPSILON) * gain
        if i < G:
            ho[n] = mixed.astype(BF16)
            ho_out(i).start()
        else:
            hr[g] = mixed.astype(BF16)
    loads[5].wait()
    for i in range(1, G):
        o = (g + i) % G
        remote(hr.at[o], hr.at[o], ho_s.at[i], ho_r.at[o], s, t).wait_recv()

    def branch_rows(o):
        at = pl.multiple_of(o * rows, rows)
        mine = jnp.concatenate([hr[i, pl.ds(at, rows), :] for i in range(G)], axis=1)
        return jnp.dot(mine, wo[...], preferred_element_type=F32)

    def rs_out(i):
        o = (t + i) % T
        return remote(rsend.at[o], rs.at[t], rs_s.at[i], rs_r.at[t], s, o)

    for i in range(1, T):
        o = (t + i) % T
        rsend[o] = branch_rows(o).astype(BF16)
        rs_out(i).start()
    branch = branch_rows(t)
    for i in range(1, T):
        o = (t + i) % T
        remote(rs.at[o], rs.at[o], rs_s.at[i], rs_r.at[o], s, o).wait_recv()
        branch = branch + rs[o].astype(F32)
    out_ref[...] = (latent_ref[...].astype(F32) + modrow[0:1, 2 * D :] * branch).astype(BF16)

    for i in range(1, T):
        part_copy(i).wait_send()
        latent_copy(i).wait_send()
        rs_out(i).wait_send()

    @pl.loop(1, S)
    def _(i):
        mod_copy(i, s).wait_send()

    for i in range(1, G):
        kv_out(i).wait_send()
        q_out(i).wait_send()
        ho_out(i).wait_send()
    for i in range(G):

        @pl.loop(1, R)
        def _(j):
            forward(i, j).wait_send()


def body(
    S, T,
    latent, context, condition, context_condition, modulation_weight,
    query_first, query_second, key_first, key_second, value_weight,
    lambda_head, context_score_boost, head_gain, output_weight,
):
    rows, D = latent.shape
    Lr = rows * T
    G = value_weight.shape[1] // VALUE_DIM
    assert S % G == 0
    R = S // G
    B = math.gcd(R, 4)
    Cr = context.shape[0]
    Cp = -(-Cr // 16) * 16
    if Cp != Cr:
        context = jnp.pad(context, ((0, Cp - Cr), (0, 0)))
    cw = modulation_weight.shape[1]
    cp = -(-cw // LANES) * LANES
    if cp != cw:
        modulation_weight = jnp.pad(modulation_weight, ((0, 0), (0, cp - cw)))
    depth = modulation_weight.shape[0]
    positions = lax.axis_index("sp") * Lr + jnp.arange(Lr, dtype=jnp.int32)
    cosine, sine = rotation_tables(positions, Cp)
    vm = pl.BlockSpec(memory_space=pltpu.VMEM)
    sm = pl.BlockSpec(memory_space=pltpu.SMEM)
    hb = pl.BlockSpec(memory_space=pl.ANY)
    V = pltpu.VMEM
    dma = pltpu.SemaphoreType.DMA
    weights = (query_first, query_second, key_first, key_second, value_weight, output_weight)
    return pl.pallas_call(
        functools.partial(kernel, (S, T, G, R, B, Cr, cw)),
        out_shape=jax.ShapeDtypeStruct((rows, D), BF16),
        in_specs=[vm] * 5 + [hb] * 5 + [sm, sm, vm, hb, vm, vm],
        out_specs=vm,
        scratch_shapes=[V(w.shape, BF16) for w in weights]
        + [
            V((2, depth), F32),
            V((T, 2, cp), F32),
            V((S, 2, cp), F32),
            V((2, 3 * D), F32),
            V((T, rows, D), BF16),
            V((Lr + Cp, D), BF16),
            V((G, Lr, LANES), BF16),
            V((G, Lr + Cp, LANES + VALUE_DIM), BF16),
            V((G, Lr, LANES), BF16),
            V((S, Lr + Cp, LANES + VALUE_DIM), BF16),
            V((2, G, Lr, 1), F32),
            V((2, G, Lr, 1), F32),
            V((2, G, Lr, VALUE_DIM), F32),
            V((G, Lr, VALUE_DIM), BF16),
            V((G, Lr, VALUE_DIM), BF16),
            V((T, rows, D), BF16),
            V((T, rows, D), BF16),
            dma((6,)),
            dma((T,)), dma((T,)), dma((T,)), dma((T,)), dma((S,)), dma((S,)),
            dma((G,)), dma((G,)), dma((G,)), dma((G, R)), dma((S,)),
            dma((G,)), dma((G,)), dma((T,)), dma((T,)),
        ],
        compiler_params=pltpu.CompilerParams(
            collective_id=0, has_side_effects=True, vmem_limit_bytes=62 * 1024 * 1024
        ),
    )(
        latent, context, condition[None, :], context_condition[None, :], modulation_weight,
        query_first, query_second, key_first, key_second, value_weight,
        lambda_head, context_score_boost, head_gain[None, :], output_weight, cosine, sine,
    )


def solution(mesh):
    in_specs = (
        P(("sp", "tp"), None),
        P("sp", None),
        P("tp"),
        P("tp"),
        P("tp", "sp"),
        P(None, "tp"),
        P(None, "tp"),
        P(None, "tp"),
        P(None, "tp"),
        P(None, "tp"),
        P("tp"),
        P("tp"),
        P(),
        P("tp", None),
    )
    out_specs = P(("sp", "tp"), None)
    run = functools.partial(body, mesh.shape["sp"], mesh.shape["tp"])
    return jax.shard_map(run, mesh=mesh, in_specs=in_specs, out_specs=out_specs, check_vma=False)
```

```python
import functools
import math

import jax
import jax.numpy as jnp
import numpy as np
from jax import lax
from jax.experimental import pallas as pl
from jax.experimental.pallas import tpu as pltpu
from jax.sharding import PartitionSpec as P

HEAD_DIM = 64
VALUE_DIM = 128
GRID_W = 64
EPSILON = 1e-06
THETA = 10000.0
NEGATIVE = -1e30
LOG2E = math.log2(math.e)
MESH = pl.DeviceIdType.MESH
BF16 = jnp.bfloat16
F32 = jnp.float32
LANES = 128
QROWS = 256


def rotation_tables(grid_rows):
    half = HEAD_DIM // 2
    quarter = half // 2
    lane = np.arange(LANES) % HEAD_DIM
    rate = (THETA ** (-(lane % quarter) / quarter)).astype(np.float32)
    sign = np.where(lane % half < quarter, -1.0, 1.0)
    tables = []
    for count, mask in ((grid_rows, lane < half), (GRID_W, lane >= half)):
        angle = np.arange(count, dtype=np.float32)[:, None] * rate[None, :]
        for table in (np.cos(angle), np.sin(angle) * sign):
            tables.append(np.where(mask, table, 0.0).astype(np.float32))
    return tables


def rotate(x, cosine, sine):
    quarter = HEAD_DIM // 4
    lane = lax.broadcasted_iota(jnp.int32, x.shape, 1)
    ahead = pltpu.roll(x, LANES - quarter, 1)
    behind = pltpu.roll(x, quarter, 1)
    flipped = jnp.where(lane % (2 * quarter) < quarter, ahead, behind)
    return x * cosine + flipped * sine


def normed_rows(rows):
    v = rows.astype(F32)
    return v * lax.rsqrt(jnp.mean(v * v, axis=-1, keepdims=True) + EPSILON)


def kernel(
    dims,
    latent_ref, context_ref, cond_ref, ccond_ref, modw_ref,
    wq1_hbm, wq2_hbm, wk1_hbm, wk2_hbm, wv_hbm,
    lam_ref, boost_ref, gain_ref, wo_hbm, crow_ref, srow_ref, ccol_ref, scol_ref,
    out_ref,
    wq1, wq2, wk1, wk2, wv, wo,
    cos_ref, sin_ref, sig, modp, modall, modrow, lat, nrm, h,
    qs, kvs, q, kv, mx, acc, ho, hr, rsend, rs,
    wsem, mp_s, mp_r, lt_s, lt_r, ma_s, ma_r,
    q_s, q_r, kz_s, kv_s, kv_r, ho_s, ho_r, rs_s, rs_r,
):
    S, T, G, R, B, Cr, cw = dims
    s, t = lax.axis_index("sp"), lax.axis_index("tp")
    g, r = s // R, s % R
    rows, D = latent_ref.shape
    Lr = rows * T
    Cp = context_ref.shape[0]

    def remote(src, dst, send, recv, sp, tp):
        return pltpu.make_async_remote_copy(
            src_ref=src, dst_ref=dst, send_sem=send, recv_sem=recv,
            device_id=(sp, tp), device_id_type=MESH,
        )

    loads = [
        pltpu.make_async_copy(a, b, wsem.at[i])
        for i, (a, b) in enumerate(
            [(wq1_hbm, wq1), (wq2_hbm, wq2), (wk1_hbm, wk1), (wk2_hbm, wk2), (wv_hbm, wv), (wo_hbm, wo)]
        )
    ]
    for load in loads:
        load.start()

    barrier = pltpu.get_barrier_semaphore()

    @pl.loop(1, S)
    def _(i):
        pl.semaphore_signal(barrier, inc=1, device_id=((s + i) % S, t), device_id_type=MESH)

    for i in range(1, T):
        pl.semaphore_signal(barrier, inc=1, device_id=(s, (t + i) % T), device_id_type=MESH)

    for i in range(Lr // GRID_W):
        span, at = slice(i * GRID_W, (i + 1) * GRID_W), pl.ds(s * (Lr // GRID_W) + i, 1)
        cos_ref[span, :] = ccol_ref[...] + crow_ref[at, :]
        sin_ref[span, :] = scol_ref[...] + srow_ref[at, :]
    cos_ref[Lr:, :] = jnp.ones((Cp, LANES), F32)
    sin_ref[Lr:, :] = jnp.zeros((Cp, LANES), F32)

    for i, ref in enumerate((cond_ref, ccond_ref)):
        v = ref[...]
        sig[i : i + 1, :] = v / (1.0 + jnp.exp(-v))
    modp[t] = jnp.dot(sig[...].astype(BF16), modw_ref[...], preferred_element_type=F32)

    pl.semaphore_wait(barrier, S - 1 + T - 1)

    def part_copy(i):
        return remote(modp.at[t], modp.at[t], mp_s.at[i], mp_r.at[t], s, (t + i) % T)

    def latent_copy(i):
        return remote(latent_ref, lat.at[t], lt_s.at[i], lt_r.at[t], s, (t + i) % T)

    for i in range(1, T):
        part_copy(i).start()
    for i in range(1, T):
        latent_copy(i).start()
    lat[t] = latent_ref[...]
    for i in range(1, T):
        o = (t + i) % T
        remote(modp.at[o], modp.at[o], mp_s.at[i], mp_r.at[o], s, o).wait_recv()
    total = modp[0]
    for i in range(1, T):
        total = total + modp[i]
    modall[s] = total

    def mod_copy(i, src):
        return remote(modall.at[src], modall.at[src], ma_s.at[i], ma_r.at[src], (s + i) % S, t)

    @pl.loop(1, S)
    def _(i):
        mod_copy(i, s).start()

    for i in range(1, T):
        o = (t + i) % T
        remote(lat.at[o], lat.at[o], lt_s.at[i], lt_r.at[o], s, o).wait_recv()
    step = math.gcd(rows, 32)
    for i in range(T):

        @pl.loop(0, rows // step)
        def _(j):
            at = pl.multiple_of(j * step, step)
            nrm[pl.ds(i * rows + at, step), :] = normed_rows(lat[i, pl.ds(at, step), :])

    nrm[Lr:, :] = normed_rows(context_ref[...])

    @pl.loop(1, S)
    def _(i):
        mod_copy(i, (s + i) % S).wait_recv()

    for i in range(S):
        modrow[:, i * cw : (i + 1) * cw] = modall[i][:, :cw]

    @pl.loop(0, Lr // step)
    def _(j):
        at = pl.ds(pl.multiple_of(j * step, step), step)
        h[at, :] = (nrm[at, :] * (1.0 + modrow[0:1, D : 2 * D]) + modrow[0:1, :D]).astype(BF16)

    h[Lr:, :] = (nrm[Lr:, :] * (1.0 + modrow[1:2, D : 2 * D]) + modrow[1:2, :D]).astype(BF16)

    for i in range(2):
        loads[i].wait()
    lh = h[:Lr, :]
    one = jnp.dot(lh, wq1[...], preferred_element_type=F32)
    two = jnp.dot(lh, wq2[...], preferred_element_type=F32)
    for i in range(G):
        cut = slice(i * HEAD_DIM, (i + 1) * HEAD_DIM)
        pair = jnp.concatenate([one[:, cut], two[:, cut]], axis=1)
        turned = rotate(pair, cos_ref[:Lr, :], sin_ref[:Lr, :])
        qs[i] = (turned * (LOG2E * HEAD_DIM**-0.5)).astype(BF16)

    def q_out(i):
        to = (g + i) % G
        return remote(qs.at[to], q.at[g], q_s.at[i], q_r.at[g], to * R + r, t)

    for i in range(1, G):
        q_out(i).start()
    q[g] = qs[g]

    for i in range(2, 5):
        loads[i].wait()
    hh = h[...]
    one = jnp.dot(hh, wk1[...], preferred_element_type=F32)
    two = jnp.dot(hh, wk2[...], preferred_element_type=F32)
    for i in range(G):
        cut = slice(i * HEAD_DIM, (i + 1) * HEAD_DIM)
        pair = jnp.concatenate([one[:, cut], two[:, cut]], axis=1)
        kvs[i, :, :LANES] = rotate(pair, cos_ref[...], sin_ref[...]).astype(BF16)
    val = jnp.dot(hh, wv[...], preferred_element_type=F32)
    for i in range(G):
        kvs[i, :, LANES:] = val[:, i * VALUE_DIM : (i + 1) * VALUE_DIM].astype(BF16)

    def kv_out(i):
        to = (g + i) % G
        return remote(kvs.at[to], kv.at[s], kz_s.at[i], kv_r.at[s], to * R + r, t)

    for i in range(1, G):
        kv_out(i).start()
    kv[s] = kvs[g]

    def forward(i, j):
        src = ((g + G - i) % G) * R + r
        return remote(kv.at[src], kv.at[src], kv_s.at[i, j], kv_r.at[src], g * R + (r + j) % R, t)

    def landed(src):
        remote(kv.at[src], kv.at[src], kz_s.at[0], kv_r.at[src], s, t).wait_recv()

    def forward_all(i):
        @pl.loop(1, R)
        def _(j):
            forward(i, j).start()

    forward_all(0)
    mx[...] = jnp.full(mx.shape, NEGATIVE, F32)
    acc[...] = jnp.zeros(acc.shape, F32)
    boost = boost_ref[g] * LOG2E

    for i in range(1, G):
        o = (g + i) % G
        remote(q.at[o], q.at[o], q_s.at[i], q_r.at[o], s, t).wait_recv()

    def attend(n, at):
        k_l = kv[pl.ds(at, B), :Lr, :LANES].reshape(B * Lr, LANES)
        v_l = kv[pl.ds(at, B), :Lr, LANES:].reshape(B * Lr, VALUE_DIM)
        k_c = kv[pl.ds(at, B), Lr:, :LANES].reshape(B * Cp, LANES)
        v_c = kv[pl.ds(at, B), Lr:, LANES:].reshape(B * Cp, VALUE_DIM)
        v_l = jnp.concatenate([v_l, jnp.ones_like(v_l)], axis=1)
        v_c = jnp.concatenate([v_c, jnp.ones_like(v_c)], axis=1)
        nt = (((1,), (1,)), ((), ()))
        QB = min(Lr, QROWS)
        for m, c in [(m, c) for c in range(Lr // QB) for m in range(2)]:
            part = slice(c * QB, (c + 1) * QB)
            qq = q[n, part, :]
            lane = lax.broadcasted_iota(jnp.int32, qq.shape, 1)
            qm = jnp.where(lane // HEAD_DIM == m, qq, jnp.zeros_like(qq))
            s_l = lax.dot_general(qm, k_l, nt, preferred_element_type=F32)
            s_c = lax.dot_general(qm, k_c, nt, preferred_element_type=F32) + boost
            if Cp != Cr:
                spot = lax.broadcasted_iota(jnp.int32, s_c.shape, 1)
                s_c = jnp.where(spot % Cp < Cr, s_c, NEGATIVE)
            old = mx[m, n, part, :]
            peak = jnp.maximum(
                old,
                jnp.maximum(
                    jnp.max(s_l, axis=-1, keepdims=True), jnp.max(s_c, axis=-1, keepdims=True)
                ),
            )
            p_l = jnp.exp2(s_l - peak).astype(BF16)
            p_c = jnp.exp2(s_c - peak).astype(BF16)
            mx[m, n, part, :] = peak
            acc[m, n, part, :] = (
                jnp.exp2(old - peak) * acc[m, n, part, :]
                + jnp.dot(p_l, v_l, preferred_element_type=F32)
                + jnp.dot(p_c, v_c, preferred_element_type=F32)
            )

    lam = lam_ref[g]
    gain = gain_ref[...]

    def finish(n):
        one = acc[0, n, :, :VALUE_DIM] / acc[0, n, :, VALUE_DIM:]
        two = acc[1, n, :, :VALUE_DIM] / acc[1, n, :, VALUE_DIM:]
        mixed = one - lam * two
        mixed = mixed * lax.rsqrt(jnp.mean(mixed * mixed, axis=-1, keepdims=True) + EPSILON) * gain
        return mixed.astype(BF16)

    def ho_out(i):
        to = (g + i) % G
        return remote(ho.at[to], hr.at[g], ho_s.at[i], ho_r.at[g], to * R + r, t)

    def pass_on(i):
        landed(((g + G - i) % G) * R + r)
        forward_all(i)

    for i in range(G):
        if i == 1 and G > 2:
            pass_on(2)
        base = ((g + G - i) % G) * R

        @pl.loop(1, R)
        def _(j):
            landed(base + (r + j) % R)

        if i + 1 < G:
            half = G // 2
            for low, high in ((0, half), (half, G)):
                if low and i == 0:
                    pass_on(1)
                elif low and i + 2 < G:
                    pass_on(i + 2)

                @pl.loop(low * (R // B), high * (R // B))
                def _(x):
                    attend(x // (R // B), base + x % (R // B) * B)

        else:

            @pl.loop(1, G + 1)
            def _(y):
                n = (g + y) % G

                @pl.loop(0, R // B)
                def _(x):
                    attend(n, base + x * B)

                ho[n] = finish(n)

                @pl.when(y < G)
                def _():
                    ho_out(y).start()

    hr[g] = ho[g]
    loads[5].wait()
    for i in range(1, G):
        o = (g + i) % G
        remote(hr.at[o], hr.at[o], ho_s.at[i], ho_r.at[o], s, t).wait_recv()

    def branch_rows(o):
        at = pl.multiple_of(o * rows, rows)
        mine = jnp.concatenate([hr[i, pl.ds(at, rows), :] for i in range(G)], axis=1)
        return jnp.dot(mine, wo[...], preferred_element_type=F32)

    def rs_out(i):
        o = (t + i) % T
        return remote(rsend.at[o], rs.at[t], rs_s.at[i], rs_r.at[t], s, o)

    for i in range(1, T):
        o = (t + i) % T
        rsend[o] = branch_rows(o).astype(BF16)
        rs_out(i).start()
    branch = branch_rows(t)
    for i in range(1, T):
        o = (t + i) % T
        remote(rs.at[o], rs.at[o], rs_s.at[i], rs_r.at[o], s, o).wait_recv()
        branch = branch + rs[o].astype(F32)
    out_ref[...] = (latent_ref[...].astype(F32) + modrow[0:1, 2 * D :] * branch).astype(BF16)

    for i in range(1, T):
        part_copy(i).wait_send()
        latent_copy(i).wait_send()
        rs_out(i).wait_send()

    @pl.loop(1, S)
    def _(i):
        mod_copy(i, s).wait_send()

    for i in range(1, G):
        kv_out(i).wait_send()
        q_out(i).wait_send()
        ho_out(i).wait_send()
    for i in range(G):

        @pl.loop(1, R)
        def _(j):
            forward(i, j).wait_send()


def body(
    S, T,
    latent, context, condition, context_condition, modulation_weight,
    query_first, query_second, key_first, key_second, value_weight,
    lambda_head, context_score_boost, head_gain, output_weight,
):
    rows, D = latent.shape
    Lr = rows * T
    G = value_weight.shape[1] // VALUE_DIM
    assert S % G == 0
    R = S // G
    B = math.gcd(R, 4)
    Cr = context.shape[0]
    Cp = -(-Cr // 16) * 16
    if Cp != Cr:
        context = jnp.pad(context, ((0, Cp - Cr), (0, 0)))
    cw = modulation_weight.shape[1]
    cp = -(-cw // LANES) * LANES
    if cp != cw:
        modulation_weight = jnp.pad(modulation_weight, ((0, 0), (0, cp - cw)))
    depth = modulation_weight.shape[0]
    assert Lr % GRID_W == 0
    tables = rotation_tables(S * Lr // GRID_W)
    vm = pl.BlockSpec(memory_space=pltpu.VMEM)
    sm = pl.BlockSpec(memory_space=pltpu.SMEM)
    hb = pl.BlockSpec(memory_space=pl.ANY)
    V = pltpu.VMEM
    dma = pltpu.SemaphoreType.DMA
    weights = (query_first, query_second, key_first, key_second, value_weight, output_weight)
    return pl.pallas_call(
        functools.partial(kernel, (S, T, G, R, B, Cr, cw)),
        out_shape=jax.ShapeDtypeStruct((rows, D), BF16),
        in_specs=[vm] * 5 + [hb] * 5 + [sm, sm, vm, hb, vm, vm, vm, vm],
        out_specs=vm,
        scratch_shapes=[V(w.shape, BF16) for w in weights]
        + [
            V((Lr + Cp, LANES), F32),
            V((Lr + Cp, LANES), F32),
            V((2, depth), F32),
            V((T, 2, cp), F32),
            V((S, 2, cp), F32),
            V((2, 3 * D), F32),
            V((T, rows, D), BF16),
            V((Lr + Cp, D), F32),
            V((Lr + Cp, D), BF16),
            V((G, Lr, LANES), BF16),
            V((G, Lr + Cp, LANES + VALUE_DIM), BF16),
            V((G, Lr, LANES), BF16),
            V((S, Lr + Cp, LANES + VALUE_DIM), BF16),
            V((2, G, Lr, 1), F32),
            V((2, G, Lr, 2 * VALUE_DIM), F32),
            V((G, Lr, VALUE_DIM), BF16),
            V((G, Lr, VALUE_DIM), BF16),
            V((T, rows, D), BF16),
            V((T, rows, D), BF16),
            dma((6,)),
            dma((T,)), dma((T,)), dma((T,)), dma((T,)), dma((S,)), dma((S,)),
            dma((G,)), dma((G,)), dma((G,)), dma((G, R)), dma((S,)),
            dma((G,)), dma((G,)), dma((T,)), dma((T,)),
        ],
        compiler_params=pltpu.CompilerParams(
            collective_id=0, has_side_effects=True, vmem_limit_bytes=62 * 1024 * 1024
        ),
    )(
        latent, context, condition[None, :], context_condition[None, :], modulation_weight,
        query_first, query_second, key_first, key_second, value_weight,
        lambda_head, context_score_boost, head_gain[None, :], output_weight, *tables,
    )


def solution(mesh):
    in_specs = (
        P(("sp", "tp"), None),
        P("sp", None),
        P("tp"),
        P("tp"),
        P("tp", "sp"),
        P(None, "tp"),
        P(None, "tp"),
        P(None, "tp"),
        P(None, "tp"),
        P(None, "tp"),
        P("tp"),
        P("tp"),
        P(),
        P("tp", None),
    )
    out_specs = P(("sp", "tp"), None)
    run = functools.partial(body, mesh.shape["sp"], mesh.shape["tp"])
    return jax.shard_map(run, mesh=mesh, in_specs=in_specs, out_specs=out_specs, check_vma=False)
```
